256 devices in a mesh: grp: 2 (over y), ep: 64 (over z, x), tp: 2 (over core).
Axes of the slice: x: 4, y: 2, z: 16, core: 2. Of those that a mesh axis runs over, the one named last changes fastest.
The devices are a block of a 4x16x16 slice.
Arguments:
- tokens: bfloat16 [16384, 2048], P(('grp', 'ep')), parts along dimension 0, may hold values from -6 to 6
- in_gain: float32 [2048], replicated, may hold values from 0.1 to 1.9
- routing: int32 [16384, 4], P(('grp', 'ep')), parts along dimension 0, may hold values from 0 to 127, as said below
- gate_prob: float32 [16384, 4], P(('grp', 'ep')), parts along dimension 0, may hold values from 0.05 to 1
- w_gate: bfloat16 [128, 2048, 512], P('ep', None, 'tp'), may hold values from -0.125 to 0.125
- w_up: bfloat16 [128, 2048, 512], P('ep', None, 'tp'), may hold values from -0.125 to 0.125
- w_down: bfloat16 [128, 512, 2048], P('ep', 'tp')
- out_gain: float32 [2048], P('tp'), may hold values from 0.1 to 1.9
Outputs:
- output: bfloat16 [16384, 2048], P(('grp', 'ep'), 'tp'), parts along dimension 0
The draws below stay inside these ranges and needn't reach their ends.
There are 2 independent parts, one for each index of `grp`. The reference program is written for one: setup_inputs(seed, part) draws one part's arguments, and reference() takes and returns one part's arrays. A program takes and returns all parts, laid end to end along the dimension named above; an argument that names none is the same for every part. Nothing has to cross between parts.
Inputs may be any that keep to these rules, and one draw needn't show every extreme that they name: `routing`: each row names 4 different experts, all of one group (the same value of expert // 32). In the rows of one device no expert is named more than 8 times, and in every device's rows some expert is named exactly 8 times.
All inputs are finite; a program needn't handle non-finite values.
Results may differ from the reference program's by a relative error of at most 0.0077.
Values may be sent and summed in bfloat16 or wider, within the bound.
No kernel may reach another device: no remote copies, remote signals or barrier semaphores. Data moves between devices by JAX's collectives and lax.ppermute only.
A program may use at most 64 MiB of HBM per device.

```python
import math
import jax
import jax.numpy as jnp
from jax import lax

D = 2048
FF = 512
GROUPS = 4
TOPK = 4
TOK_DEV = 128
EXPERTS = 128
EPG = 32
TOKENS = 8192
CAP = 8
GMAX = 64
N_EP = 64
N_TP = 2


def draw_routing(key, part):
    block_count = TOKENS // TOK_DEV
    key_order, key_pick, key_perm, key_shuffle = jax.random.split(key, 4)
    hot_count = min(GMAX, TOK_DEV)
    hot_span = hot_count * TOPK // CAP
    group_order = jax.random.permutation(key_order, GROUPS)
    hot_picks = jnp.minimum(jax.random.randint(key_pick, (block_count,), 0, GROUPS + 2), GROUPS - 1)
    hot_group = group_order[hot_picks]
    position = jnp.arange(TOK_DEV, dtype=jnp.int32)
    is_hot = position < hot_count
    cold_index = position - hot_count
    groups = jnp.where(is_hot[None, :], hot_group[:, None], (hot_group[:, None] + 1 + cold_index[None, :] % (GROUPS - 1)) % GROUPS)
    group_rank = jnp.where(is_hot, position, cold_index // (GROUPS - 1))
    modulus = jnp.where(is_hot, hot_span, EPG)
    within = (group_rank[:, None] * TOPK + jnp.arange(TOPK, dtype=jnp.int32)[None, :]) % modulus[:, None]
    perm_keys = jax.random.split(key_perm, block_count * GROUPS)
    orders = jax.vmap(lambda one_key: jax.random.permutation(one_key, EPG))(perm_keys).reshape(block_count, GROUPS, EPG)
    block_ids = jnp.arange(block_count)[:, None, None]
    local_ids = orders[block_ids, groups[:, :, None], within[None, :, :]]
    experts = groups[:, :, None] * EPG + local_ids
    shuffle_keys = jax.random.split(key_shuffle, block_count)
    shuffles = jax.vmap(lambda one_key: jax.random.permutation(one_key, TOK_DEV))(shuffle_keys)
    experts = jnp.take_along_axis(experts, shuffles[:, :, None], axis=1)
    return experts.reshape(TOKENS, TOPK).astype(jnp.int32)


def draw_w_down(key, part):
    key_base, key_col = jax.random.split(key)
    columns = jnp.arange(D, dtype=jnp.float32) / D
    entries_base = jax.random.normal(key_base, (EXPERTS, FF, D), jnp.float32)
    spread = jax.random.uniform(key_col, (D,), jnp.float32, 0.5, 1.5)
    col_rise = 3.0 ** columns
    return (entries_base * FF ** (-0.5) * col_rise * spread).astype(jnp.bfloat16)


def levels(own_key, dims, cuts, low, largest):
    def one(dim, parts):
        draws = jax.random.uniform(jax.random.fold_in(jax.random.fold_in(own_key, 6), dim), (parts,), jnp.float32, low / len(cuts), largest / len(cuts))
        return jnp.repeat(jnp.exp(draws), dims[dim] // parts).reshape((-1,) + (1,) * (len(dims) - dim - 1))

    gain = one(*cuts[0])
    for cut in cuts[1:]:
        gain = gain * one(*cut)
    return gain


def bell_draw(rng, extent, width, most, cuts=(), kind=jnp.bfloat16):
    result = jax.random.normal(rng, extent, jnp.float32) * width
    if len(cuts) > 0:
        result = levels(rng, extent, cuts, -0.22, 0.18) * result
    return jnp.clip(result, min=-most, max=most).astype(kind)


def setup_inputs(seed: int = 0, part: int = 0) -> dict:
    seeds = jax.random.split(jax.random.key(seed), 9)
    part_keys = jax.random.split(jax.random.fold_in(seeds[8], part), 9)
    tokens = bell_draw(part_keys[0], (TOKENS, D), 1.0, 6.0, ((0, 64),))
    in_gain = jnp.clip(1.0 + 0.18 * jax.random.normal(seeds[1], (D,), jnp.float32), 0.1, 1.9)
    routing = draw_routing(jax.random.fold_in(jax.random.fold_in(seeds[8], part), 71), part)
    gate_prob = jnp.clip(jnp.exp(math.log(1.0) - 2.9957323 * jax.random.uniform(part_keys[3], (TOKENS, TOPK), jnp.float32) ** levels(part_keys[3], (TOKENS, TOPK), ((0, 64),), -0.2, 0.2)), 0.05, 1.0)
    w_gate = bell_draw(seeds[4], (EXPERTS, D, FF), D ** -0.5, 0.125, ((0, 64), (2, 2)))
    w_up = bell_draw(seeds[5], (EXPERTS, D, FF), D ** -0.5, 0.125, ((0, 64), (2, 2)))
    w_down = draw_w_down(jax.random.fold_in(seeds[8], 71), part)
    out_gain = jnp.clip(1.0 + 0.18 * jax.random.normal(seeds[7], (D,), jnp.float32), 0.1, 1.9)
    return dict(tokens=tokens, in_gain=in_gain, routing=routing, gate_prob=gate_prob, w_gate=w_gate, w_up=w_up, w_down=w_down, out_gain=out_gain)


EPS = 1e-06

def slot_ranks(flat_routes):
    matches = (flat_routes[:, None] == jnp.arange(EXPERTS, dtype=jnp.int32)[None, :]).astype(jnp.int32)
    earlier = jnp.cumsum(matches, axis=0) - matches
    return lax.optimization_barrier(jnp.sum(earlier * matches, axis=1)).astype(jnp.int32)

def reference(tokens, in_gain, routing, gate_prob, w_gate, w_up, w_down, out_gain):
    floats = tokens.astype(jnp.float32)
    normed = (floats * lax.rsqrt(lax.optimization_barrier(jnp.mean(floats * floats, axis=-1, keepdims=True)) + EPS) * in_gain).astype(jnp.bfloat16)
    blocks = routing.reshape(N_EP, TOK_DEV * TOPK)
    slot_rank = jax.vmap(slot_ranks)(blocks)
    sources = jnp.arange(N_EP, dtype=jnp.int32)[:, None]
    slot_ids = (blocks * (N_EP * CAP) + sources * CAP + slot_rank).reshape(-1).astype(jnp.int32)
    token_ids = jnp.arange(TOKENS * TOPK, dtype=jnp.int32) // TOPK
    slot_table = jnp.zeros((EXPERTS * N_EP * CAP,), jnp.int32).at[slot_ids].set(token_ids + 1)
    slot_table = slot_table.reshape(EXPERTS, N_EP * CAP)

    def expert(inputs):
        entries, gate_w, up_w, down_w = inputs
        filled = entries > 0
        rows_in = jnp.where(filled[:, None], normed[jnp.maximum(entries - 1, 0)], jnp.zeros((), jnp.bfloat16))
        gate_act = jnp.dot(rows_in, gate_w, preferred_element_type=jnp.float32)
        up_act = jnp.dot(rows_in, up_w, preferred_element_type=jnp.float32)
        hidden = (jax.nn.silu(gate_act) * up_act).astype(jnp.bfloat16)
        pieces = jnp.einsum('rnf,nfd->nrd', hidden.reshape(-1, N_TP, FF // N_TP).astype(jnp.float32), down_w.reshape(N_TP, FF // N_TP, D).astype(jnp.float32))
        rounded = lax.optimization_barrier(pieces.astype(jnp.bfloat16))
        return lax.optimization_barrier(jnp.sum(rounded.astype(jnp.float32), axis=0)).astype(jnp.bfloat16)
    results = lax.map(expert, (slot_table, w_gate, w_up, w_down))
    picked = results.reshape(-1, D)[slot_ids].astype(jnp.float32).reshape(TOKENS, TOPK, D)
    mixed_rows = lax.optimization_barrier(jnp.sum(picked * gate_prob[:, :, None], axis=1))
    inv_rms = lax.rsqrt(lax.optimization_barrier(jnp.mean(mixed_rows * mixed_rows, axis=-1, keepdims=True)) + EPS)
    return (mixed_rows * inv_rms * out_gain).astype(jnp.bfloat16)
```

```python
import functools

import jax
import jax.numpy as jnp
from jax import lax
from jax.experimental import pallas as pl
from jax.experimental.pallas import tpu as pltpu
from jax.sharding import Mesh, PartitionSpec as P

GROUPS = 4
X_CHIPS = 4
EPS = 1e-06
META = 8


f32 = jnp.float32
bf16 = jnp.bfloat16
VM = pl.BlockSpec(memory_space=pltpu.VMEM)
SM = pl.BlockSpec(memory_space=pltpu.SMEM)
HB = pl.BlockSpec(memory_space=pl.ANY)


def iota(shape, dim):
    return lax.broadcasted_iota(jnp.int32, shape, dim)


def prep_kernel(expert_count, place, tokens, gain, routes, gates, *outs):
    core = place[0]
    half = tokens.shape[1] // 2
    rows = tokens.shape[0]
    top = routes.shape[0]
    chunk = outs[0].shape[1]
    x = tokens[...].astype(f32)
    scale = lax.rsqrt(jnp.mean(x * x, axis=-1, keepdims=True) + EPS)
    start = pl.multiple_of(core * half, half)
    own = tokens[:, pl.ds(start, half)].astype(f32)
    normed = (own * scale * gain[:, pl.ds(start, half)]).astype(bf16)
    before = (iota((rows, rows), 0) < iota((rows, rows), 1)).astype(bf16)
    names = iota((expert_count, rows), 0)
    base = jnp.zeros((expert_count, 1), f32)
    ranks = []
    for k in range(top):
        hit = names == routes[k : k + 1, :]
        hits = hit.astype(bf16)
        earlier = jnp.dot(hits, before, preferred_element_type=f32) + base
        ranks.append(jnp.sum(jnp.where(hit, earlier, 0.0), axis=0, keepdims=True))
        base = base + jnp.sum(hits.astype(f32), axis=1, keepdims=True)
    g = gates[...]
    high = g.astype(bf16)
    low = (g - high.astype(f32)).astype(bf16)

    def lanes(pieces):
        return jnp.concatenate([p.astype(f32) for p in pieces], axis=1)

    route_rows = routes[...].astype(f32)
    first = [
        lanes([route_rows[k : k + 1] for k in range(top)]),
        lanes(ranks),
    ]
    second = [
        lanes([high[k : k + 1] for k in range(top)]),
        lanes([low[k : k + 1] for k in range(top)]),
    ]
    for n, (out, lines) in enumerate(zip(outs, (first, second))):
        out[0:rows, :] = normed[:, n * chunk : (n + 1) * chunk]
        block = jnp.concatenate(
            lines + [jnp.zeros((META - len(lines), chunk), f32)], axis=0
        )
        out[rows : rows + META, :] = block.astype(bf16)


def pick_kernel(sources, peers, cap, place, *refs):
    core, xi, zi = place[0], place[1], place[2]
    blocks, outs, meta = refs[: 2 * sources], refs[2 * sources : -1], refs[-1]
    rows = blocks[0].shape[0] - META
    chunk = blocks[0].shape[1]
    top = chunk // rows
    plane = peers * cap
    row_ids = iota((plane, rows), 0)
    for pair in range(sources // 2):
        picked = []
        for idx in (2 * pair, 2 * pair + 1):
            a, b = blocks[2 * idx], blocks[2 * idx + 1]
            ma = a[rows : rows + META, :].astype(f32)
            mb = b[rows : rows + META, :].astype(f32)
            sel = jnp.zeros((plane, rows), jnp.bool_)
            lines = []
            for k in range(top):
                expert = ma[0:1, k * rows : (k + 1) * rows].astype(jnp.int32)
                rank = ma[1:2, k * rows : (k + 1) * rows].astype(jnp.int32)
                local = expert - zi * peers
                inside = (local >= 0) & (local < peers)
                dx = (local // 2 - xi) & (peers // 2 - 1)
                dt = (local & 1) ^ core
                rel = jnp.where(inside, (dx * 2 + dt) * cap + rank, -1)
                sel = sel | (row_ids == rel)
                lines.append(rel.astype(f32))
            for k in range(top):
                lines.append(
                    mb[0:1, k * rows : (k + 1) * rows] + mb[1:2, k * rows : (k + 1) * rows]
                )
            meta[idx * 2 * top : (idx + 1) * 2 * top, :] = jnp.concatenate(lines, axis=0)
            onehot = sel.astype(f32).astype(bf16)
            picked.append(
                [jnp.dot(onehot, m[0:rows, :], preferred_element_type=f32) for m in (a, b)]
            )
        at = 2 * pair * cap
        for p in range(peers):
            for n in range(2):
                both = jnp.concatenate(
                    [picked[i][n][p * cap : (p + 1) * cap, :] for i in range(2)], axis=0
                )
                outs[p][at : at + 2 * cap, n * chunk : (n + 1) * chunk] = both.astype(bf16)


def expert_kernel(peers, place, *refs):
    pieces, refs = refs[:peers], refs[peers:]
    weights, refs = refs[:6], refs[6:]
    outs, refs = refs[:peers], refs[peers:]
    slots, sems = refs[:6], refs[6]
    core = place[0]
    copies = []
    for n in range(6):
        copies.append(pltpu.make_async_copy(weights[n].at[core], slots[n], sems.at[n]))
        copies[-1].start()
    half = pieces[0].shape[1]
    rows = pieces[0].shape[0]
    mine = pl.multiple_of(core * half, half)
    other = pl.multiple_of((1 - core) * half, half)
    xa = jnp.concatenate([pieces[2 * d][...] for d in range(peers // 2)], axis=0)
    xb = jnp.concatenate([pieces[2 * d + 1][...] for d in range(peers // 2)], axis=0)

    def project(w):
        return jnp.dot(xa, w[pl.ds(mine, half), :], preferred_element_type=f32) + jnp.dot(
            xb, w[pl.ds(other, half), :], preferred_element_type=f32
        )

    hidden = []
    for h in range(2):
        copies[3 * h].wait()
        gate = project(slots[3 * h])
        copies[3 * h + 1].wait()
        up = project(slots[3 * h + 1])
        hidden.append((gate / (1.0 + jnp.exp(-gate)) * up).astype(bf16))
    copies[2].wait()
    copies[5].wait()
    for dt, at in enumerate((mine, other)):
        y = jnp.dot(hidden[0], slots[2][:, pl.ds(at, half)], preferred_element_type=f32)
        y = y + jnp.dot(hidden[1], slots[5][:, pl.ds(at, half)], preferred_element_type=f32)
        y = y.astype(bf16)
        for d in range(peers // 2):
            outs[2 * d + dt][...] = y[d * rows : (d + 1) * rows, :]


def mix_kernel(sources, peers, cap, *refs):
    pieces, meta, outs = refs[:peers], refs[peers], refs[peers + 1 :]
    rows = meta.shape[1]
    lines = meta.shape[0] // sources
    top = lines // 2
    chunk = outs[0].shape[1]
    plane = peers * cap
    row_ids = iota((plane, rows), 0)
    for idx in range(sources):
        m = meta[idx * lines : (idx + 1) * lines, :]
        w = jnp.zeros((plane, rows), f32)
        for k in range(top):
            w = w + jnp.where(
                row_ids == m[k : k + 1, :].astype(jnp.int32), m[top + k : top + k + 1, :], 0.0
            )
        high = w.astype(bf16)
        low = (w - high.astype(f32)).astype(bf16)
        wt = jnp.concatenate([high, low], axis=0)
        pair = (idx // 2) * 2 * cap
        off = (idx % 2) * cap
        y = jnp.concatenate(
            [
                p[pair : pair + 2 * cap, :].astype(f32)[off : off + cap, :] for p in pieces
            ],
            axis=0,
        ).astype(bf16)
        y = jnp.concatenate([y, y], axis=0)
        part = lax.dot_general(
            wt, y, (((0,), (0,)), ((), ())), preferred_element_type=f32
        )
        for n in range(2):
            out = outs[2 * idx + n]
            out[...] = part[:, n * chunk : (n + 1) * chunk].astype(out.dtype)


def shifted(value, axis, by):
    count = lax.axis_size(axis)
    return lax.ppermute(value, axis, [(i, (i + by) % count) for i in range(count)])


def swapped(value, dx, dt, back):
    xs, cores = lax.axis_size("x"), lax.axis_size("tp")
    if dx == 0 and dt == 0:
        return value
    by = -dx if back else dx
    pairs = [
        (x * cores + t, ((x + by) % xs) * cores + (t ^ dt))
        for x in range(xs)
        for t in range(cores)
    ]
    return lax.ppermute(value, ("x", "tp"), pairs)


def body(tokens, in_gain, routing, gate_prob, w_gate, w_up, w_down, out_gain):
    planes = lax.axis_size("z")
    xs = lax.axis_size("x")
    cores = lax.axis_size("tp")
    peers = xs * cores
    local_experts = w_gate.shape[0]
    expert_count = local_experts * planes * xs
    rows, top = routing.shape
    width = tokens.shape[1]
    half = out_gain.shape[0]
    chunk = half // 2
    cap = max(2, rows * top // (2 * (expert_count // GROUPS)))
    place = jnp.stack(
        [lax.axis_index("tp"), lax.axis_index("x"), lax.axis_index("z")]
    ).astype(jnp.int32)

    weights = (w_gate, w_up, w_down)
    theirs = tuple(shifted(w, "tp", 1) for w in weights)

    block = jax.ShapeDtypeStruct((rows + META, chunk), bf16)
    first = pl.pallas_call(
        functools.partial(prep_kernel, expert_count),
        out_shape=(block, block),
        in_specs=[SM, VM, VM, VM, VM],
        out_specs=(VM, VM),
        name="prep",
    )(place, tokens, in_gain.reshape(1, width), routing.T, gate_prob.T)

    reach = planes // 2
    blocks = {0: list(first)}
    up, down = list(first), list(first)
    for step in range(1, reach + 1):
        if step < reach:
            up = [shifted(v, "z", 1) for v in up]
            down = [shifted(v, "z", -1) for v in down]
            blocks[-step], blocks[step] = up, down
        else:
            blocks[reach] = [shifted(up[0], "z", 1), shifted(down[1], "z", -1)]
    order = [0, reach] + [s * k for k in range(1, reach) for s in (1, -1)]
    index = {o: i for i, o in enumerate(order)}

    piece = jax.ShapeDtypeStruct((planes * cap, half), bf16)
    picked = pl.pallas_call(
        functools.partial(pick_kernel, planes, peers, cap),
        out_shape=(piece,) * peers + (jax.ShapeDtypeStruct((planes * 2 * top, rows), f32),),
        in_specs=[SM] + [VM] * (2 * planes),
        out_specs=(VM,) * (peers + 1),
        name="pick",
    )(place, *[b for o in order for b in blocks[o]])
    meta = picked[peers]
    sent = [
        swapped(picked[2 * dx + dt], dx, dt, False) for dx in range(xs) for dt in range(cores)
    ]

    shapes = [w.shape[1:] for w in weights] * 2
    made = pl.pallas_call(
        functools.partial(expert_kernel, peers),
        out_shape=(piece,) * peers,
        in_specs=[SM] + [VM] * peers + [HB] * 6,
        out_specs=(VM,) * peers,
        scratch_shapes=[pltpu.VMEM(s, bf16) for s in shapes] + [pltpu.SemaphoreType.DMA((6,))],
        name="expert",
    )(place, *sent, *weights, *theirs)
    back = [
        swapped(made[2 * dx + dt], dx, dt, True) for dx in range(xs) for dt in range(cores)
    ]

    starts = {(reach, 0), (reach, 1), (reach - 1, 0), (1 - reach, 1)}
    parts = pl.pallas_call(
        functools.partial(mix_kernel, planes, peers, cap),
        out_shape=tuple(
            jax.ShapeDtypeStruct((rows, chunk), bf16 if (o, n) in starts else f32)
            for o in order
            for n in range(2)
        ),
        in_specs=[VM] * (peers + 1),
        out_specs=(VM,) * (2 * planes),
        name="mix",
    )(*back, meta)

    def part(offset, n):
        return parts[2 * index[offset] + n]

    sums = [part(0, n) for n in range(2)]
    flows = []
    for n, sign, length in ((0, -1, reach), (0, 1, reach - 1), (1, -1, reach - 1), (1, 1, reach)):
        far = reach if length == reach else sign * length
        flows.append([n, sign, length, part(far, n)])
    for step in range(1, reach + 1):
        for flow in flows:
            n, sign, length, value = flow
            left = length - step
            if left < 0:
                continue
            value = shifted(value, "z", sign)
            if left > 0:
                value = (value.astype(f32) + part(sign * left, n)).astype(bf16)
            flow[3] = value
    for n, _, _, value in flows:
        sums[n] = sums[n] + value.astype(f32)

    squares = sum(jnp.sum(s * s, axis=1) for s in sums)
    total = lax.all_gather(squares, "tp").sum(axis=0)
    scale = lax.rsqrt(total / width + EPS)[:, None]
    mixed = jnp.concatenate(sums, axis=1)
    return (mixed * scale * out_gain).astype(bf16)


def solution(mesh):
    grp, ep, tp = mesh.axis_names
    groups, columns, cores = mesh.devices.shape
    split = Mesh(
        mesh.devices.reshape(groups, columns // X_CHIPS, X_CHIPS, cores), (grp, "z", "x", tp)
    )
    lines = (grp, "z", "x")
    spread = ("z", "x")
    placed = (
        P(lines, None),
        P(),
        P(lines, None),
        P(lines, None),
        P(spread, None, tp),
        P(spread, None, tp),
        P(spread, tp, None),
        P(tp),
    )
    return jax.shard_map(
        body, mesh=split, in_specs=placed, out_specs=P(lines, tp), check_vma=False
    )
```

```python
import functools

import jax
import jax.numpy as jnp
from jax import lax
from jax.experimental import pallas as pl
from jax.experimental.pallas import tpu as pltpu
from jax.sharding import Mesh, PartitionSpec as P


GROUPS = 4
X_CHIPS = 4
EPS = 1e-06
NEAR = 5
META = 8
CHUNKS = 4
LIMITS = {k: v << 20 for k, v in dict(prep=62, pick=20, expert=56, mix=20).items()}


f32 = jnp.float32
bf16 = jnp.bfloat16
VM = pl.BlockSpec(memory_space=pltpu.VMEM)
SM = pl.BlockSpec(memory_space=pltpu.SMEM)
HB = pl.BlockSpec(memory_space=pl.ANY)


def iota(shape, dim):
    return lax.broadcasted_iota(jnp.int32, shape, dim)


def prep_kernel(expert_count, tokens, gain, routes, gates, *outs):
    rows = tokens.shape[0]
    top = routes.shape[0]
    chunk = outs[0].shape[1]
    x = tokens[...].astype(f32)
    scale = lax.rsqrt(jnp.mean(x * x, axis=-1, keepdims=True) + EPS)
    normed = (x * scale * gain[...]).astype(bf16)
    before = (iota((rows, rows), 0) < iota((rows, rows), 1)).astype(bf16)
    names = iota((expert_count, rows), 0)
    base = jnp.zeros((expert_count, 1), f32)
    ranks = []
    for k in range(top):
        hit = names == routes[k : k + 1, :]
        hits = hit.astype(bf16)
        earlier = jnp.dot(hits, before, preferred_element_type=f32) + base
        ranks.append(jnp.sum(jnp.where(hit, earlier, 0.0), axis=0, keepdims=True))
        base = base + jnp.sum(hits.astype(f32), axis=1, keepdims=True)
    g = gates[...]
    high = g.astype(bf16)
    low = (g - high.astype(f32)).astype(bf16)

    def lanes(pieces):
        return jnp.concatenate([p.astype(f32) for p in pieces], axis=1)

    route_rows = routes[...].astype(f32)
    lines = [
        lanes([route_rows[k : k + 1] for k in range(top)]),
        lanes(ranks),
        lanes([high[k : k + 1] for k in range(top)]),
        lanes([low[k : k + 1] for k in range(top)]),
    ]
    for n, out in enumerate(outs):
        out[0:rows, :] = normed[:, n * chunk : (n + 1) * chunk]
    block = jnp.concatenate(lines + [jnp.zeros((META - len(lines), chunk), f32)], axis=0)
    outs[0][rows : rows + META, :] = block.astype(bf16)


def pick_kernel(sources, peers, cap, place, *refs):
    blocks, out, meta = refs[: CHUNKS * sources], refs[-2], refs[-1]
    rows = blocks[0].shape[0] - META
    chunk = blocks[0].shape[1]
    top = chunk // rows
    plane = peers * cap
    row_ids = iota((plane, rows), 0)
    picked = []
    for idx in range(sources):
        mine = blocks[CHUNKS * idx : CHUNKS * (idx + 1)]
        ma = mine[0][rows : rows + META, :].astype(f32)
        sel = jnp.zeros((plane, rows), jnp.bool_)
        lines = []
        for k in range(top):
            expert = ma[0:1, k * rows : (k + 1) * rows].astype(jnp.int32)
            rank = ma[1:2, k * rows : (k + 1) * rows].astype(jnp.int32)
            local = expert - place[2] * peers
            inside = (local >= 0) & (local < peers)
            slot = jnp.where(inside, local * cap + rank, -1)
            sel = sel | (row_ids == slot)
            lines.append(slot.astype(f32))
        for k in range(top):
            lines.append(ma[2:3, k * rows : (k + 1) * rows] + ma[3:4, k * rows : (k + 1) * rows])
        meta[idx * 2 * top : (idx + 1) * 2 * top, :] = jnp.concatenate(lines, axis=0)
        onehot = sel.astype(f32).astype(bf16)
        picked.append([jnp.dot(onehot, m[0:rows, :], preferred_element_type=f32) for m in mine])
    for p in range(peers):
        for n in range(CHUNKS):
            column = [picked[i][n][p * cap : (p + 1) * cap, :] for i in range(sources)]
            out[p, :, n * chunk : (n + 1) * chunk] = jnp.concatenate(column, axis=0).astype(bf16)


def expert_kernel(place, arrived, *refs):
    weights, out, slots, sems = refs[:6], refs[6], refs[7:13], refs[13]
    core = place[0]
    copies = []
    for n in range(6):
        copies.append(pltpu.make_async_copy(weights[n].at[core], slots[n], sems.at[n]))
        copies[-1].start()
    peers, rows, _ = arrived.shape
    x = jnp.concatenate([arrived[p] for p in range(peers)], axis=0)
    hidden = []
    for h in range(2):
        copies[3 * h].wait()
        gate = jnp.dot(x, slots[3 * h][...], preferred_element_type=f32)
        copies[3 * h + 1].wait()
        up = jnp.dot(x, slots[3 * h + 1][...], preferred_element_type=f32)
        hidden.append((gate / (1.0 + jnp.exp(-gate)) * up).astype(bf16))
    copies[2].wait()
    copies[5].wait()
    y = jnp.dot(hidden[0], slots[2][...], preferred_element_type=f32)
    y = y + jnp.dot(hidden[1], slots[5][...], preferred_element_type=f32)
    y = y.astype(bf16)
    for p in range(peers):
        out[p] = y[p * rows : (p + 1) * rows, :]


def mix_kernel(sources, cap, returned, meta, *outs):
    rows = meta.shape[1]
    lines = meta.shape[0] // sources
    top = lines // 2
    chunk = outs[0].shape[1]
    peers = returned.shape[0]
    row_ids = iota((peers * cap, rows), 0)
    for idx in range(sources):
        m = meta[idx * lines : (idx + 1) * lines, :]
        w = jnp.zeros((peers * cap, rows), f32)
        for k in range(top):
            w = w + jnp.where(
                row_ids == m[k : k + 1, :].astype(jnp.int32), m[top + k : top + k + 1, :], 0.0
            )
        high = w.astype(bf16)
        low = (w - high.astype(f32)).astype(bf16)
        wt = jnp.concatenate([high, low], axis=0)
        y = jnp.concatenate(
            [returned[p, idx * cap : (idx + 1) * cap, :].astype(f32) for p in range(peers)], axis=0
        ).astype(bf16)
        y = jnp.concatenate([y, y], axis=0)
        part = lax.dot_general(wt, y, (((0,), (0,)), ((), ())), preferred_element_type=f32)
        for n in range(CHUNKS):
            out = outs[CHUNKS * idx + n]
            out[...] = part[:, n * chunk : (n + 1) * chunk].astype(out.dtype)


def shifted(value, axis, by):
    count = lax.axis_size(axis)
    return lax.ppermute(value, axis, [(i, (i + by) % count) for i in range(count)])


def moved(value, to):
    planes, cores = lax.axis_size("z"), lax.axis_size("tp")
    pairs = []
    for z in range(planes):
        for t in range(cores):
            there, core = to(z, t)
            pairs.append((z * cores + t, there % planes * cores + core))
    return lax.ppermute(value, ("z", "tp"), pairs)


def exchanged(value):
    return lax.all_to_all(value, ("x", "tp"), split_axis=0, concat_axis=0, tiled=True)


def body(tokens, in_gain, routing, gate_prob, w_gate, w_up, w_down, out_gain):
    planes = lax.axis_size("z")
    xs = lax.axis_size("x")
    cores = lax.axis_size("tp")
    peers = xs * cores
    local_experts = w_gate.shape[0]
    expert_count = local_experts * planes * xs
    rows, top = routing.shape
    width = tokens.shape[1]
    chunk = width // CHUNKS
    cap = max(2, rows * top // (2 * (expert_count // GROUPS)))
    core = lax.axis_index("tp")
    place = jnp.stack([core, lax.axis_index("x"), lax.axis_index("z")]).astype(jnp.int32)

    weights = (w_gate, w_up, w_down)
    theirs = tuple(shifted(w, "tp", 1) for w in weights)

    blank = [jax.ShapeDtypeStruct((rows + (0 if n else META), chunk), bf16) for n in range(CHUNKS)]
    held = pl.pallas_call(
        functools.partial(prep_kernel, expert_count),
        out_shape=tuple(blank),
        in_specs=[VM, VM, VM, VM],
        out_specs=(VM,) * CHUNKS,
        name="prep",
        compiler_params=pltpu.CompilerParams(vmem_limit_bytes=LIMITS["prep"]),
    )(tokens, in_gain.reshape(1, width), routing.T, gate_prob.T)

    share = planes // cores
    blocks = []
    for step in range(share):
        if step == 0:
            held = [moved(v, lambda z, t: (z + t, t)) for v in held]
        else:
            held = [moved(v, lambda z, t: (z + 2 * t - 1, t)) for v in held]
        blocks.append(held)
    near = list(range(NEAR))
    far = list(range(NEAR, share))

    def pick(offsets):
        count = len(offsets)
        return pl.pallas_call(
            functools.partial(pick_kernel, count, peers, cap),
            out_shape=(
                jax.ShapeDtypeStruct((peers, count * cap, width), bf16),
                jax.ShapeDtypeStruct((count * 2 * top, rows), f32),
            ),
            in_specs=[SM] + [VM] * (CHUNKS * count),
            out_specs=(VM, VM),
            name="pick",
            compiler_params=pltpu.CompilerParams(vmem_limit_bytes=LIMITS["pick"]),
        )(place, *[b for o in offsets for b in blocks[o]])

    def expert(arrived):
        shapes = [w.shape[1:] for w in weights] * 2
        return pl.pallas_call(
            expert_kernel,
            out_shape=jax.ShapeDtypeStruct(arrived.shape, bf16),
            in_specs=[SM, VM] + [HB] * 6,
            out_specs=VM,
            scratch_shapes=[pltpu.VMEM(s, bf16) for s in shapes] + [pltpu.SemaphoreType.DMA((6,))],
            name="expert",
            compiler_params=pltpu.CompilerParams(vmem_limit_bytes=LIMITS["expert"]),
        )(place, arrived, *weights, *theirs)

    parts = {}

    def mix(offsets, returned, meta):
        count = len(offsets)
        keys = [(o, n) for o in offsets for n in range(CHUNKS)]
        made = pl.pallas_call(
            functools.partial(mix_kernel, count, cap),
            out_shape=tuple(
                jax.ShapeDtypeStruct((rows, chunk), bf16 if k[0] == share - 1 else f32) for k in keys
            ),
            in_specs=[VM, VM],
            out_specs=(VM,) * (CHUNKS * count),
            name="mix",
            compiler_params=pltpu.CompilerParams(vmem_limit_bytes=LIMITS["mix"]),
        )(returned, meta)
        parts.update(zip(keys, made))

    near_rows, near_meta = pick(near)
    near_rows = exchanged(near_rows)
    far_rows, far_meta = pick(far)
    far_rows = exchanged(far_rows)
    near_out = expert(near_rows)
    far_out = expert(far_rows)
    far_back = exchanged(far_out)
    near_back = exchanged(near_out)
    mix(far, far_back, far_meta)
    mix(near, near_back, near_meta)

    flows = [parts[share - 1, n] for n in range(CHUNKS)]
    for step in range(1, share):
        for n in range(CHUNKS):
            value = moved(flows[n], lambda z, t: (z + 1 - 2 * t, t))
            flows[n] = (value.astype(f32) + parts[share - 1 - step, n]).astype(bf16)
    sums = []
    for n in range(CHUNKS // 2):
        low, high = flows[n], flows[n + CHUNKS // 2]
        keep = moved(jnp.where(core == 0, low, high), lambda z, t: (z - t, t))
        give = moved(jnp.where(core == 0, high, low), lambda z, t: (z - t, 1 - t))
        sums.append(keep.astype(f32) + give.astype(f32))

    squares = sum(jnp.sum(s * s, axis=1) for s in sums)
    total = lax.all_gather(squares, "tp").sum(axis=0)
    scale = lax.rsqrt(total / width + EPS)[:, None]
    mixed = jnp.concatenate(sums, axis=1)
    return (mixed * scale * out_gain).astype(bf16)


def solution(mesh):
    grp, _, tp = mesh.axis_names
    groups, columns, cores = mesh.devices.shape
    split = Mesh(
        mesh.devices.reshape(groups, columns // X_CHIPS, X_CHIPS, cores), (grp, "z", "x", tp)
    )
    lines = (grp, "z", "x")
    spread = ("z", "x")
    placed = (
        P(lines, None),
        P(),
        P(lines, None),
        P(lines, None),
        P(spread, None, tp),
        P(spread, None, tp),
        P(spread, tp, None),
        P(tp),
    )


    return jax.shard_map(body, mesh=split, in_specs=placed, out_specs=P(lines, tp), check_vma=False)
```

```python
import functools

import jax
import jax.numpy as jnp
from jax import lax
from jax.experimental import pallas as pl
from jax.experimental.pallas import tpu as pltpu
from jax.sharding import Mesh, PartitionSpec as P


GROUPS = 4
X_CHIPS = 4
EPS = 1e-06
NEAR = 6
META = 8
CHUNKS = 4
LIMITS = {k: v << 20 for k, v in dict(prep=62, pick=12, expert=56, mix=10, far_mix=62).items()}


f32 = jnp.float32
bf16 = jnp.bfloat16
VM = pl.BlockSpec(memory_space=pltpu.VMEM)
SM = pl.BlockSpec(memory_space=pltpu.SMEM)
HB = pl.BlockSpec(memory_space=pl.ANY)


def iota(shape, dim):
    return lax.broadcasted_iota(jnp.int32, shape, dim)


def prep_kernel(expert_count, tokens, gain, routes, gates, *outs):
    rows = tokens.shape[0]
    top = routes.shape[0]
    chunk = outs[0].shape[1]
    x = tokens[...].astype(f32)
    scale = lax.rsqrt(jnp.mean(x * x, axis=-1, keepdims=True) + EPS)
    normed = (x * scale * gain[...]).astype(bf16)
    before = (iota((rows, rows), 0) < iota((rows, rows), 1)).astype(bf16)
    names = iota((expert_count, rows), 0)
    base = jnp.zeros((expert_count, 1), f32)
    ranks = []
    for k in range(top):
        hit = names == routes[k : k + 1, :]
        hits = hit.astype(bf16)
        earlier = jnp.dot(hits, before, preferred_element_type=f32) + base
        ranks.append(jnp.sum(jnp.where(hit, earlier, 0.0), axis=0, keepdims=True))
        base = base + jnp.sum(hits.astype(f32), axis=1, keepdims=True)
    g = gates[...]
    high = g.astype(bf16)
    low = (g - high.astype(f32)).astype(bf16)

    def lanes(pieces):
        return jnp.concatenate([p.astype(f32) for p in pieces], axis=1)

    route_rows = routes[...].astype(f32)
    lines = [
        lanes([route_rows[k : k + 1] for k in range(top)]),
        lanes(ranks),
        lanes([high[k : k + 1] for k in range(top)]),
        lanes([low[k : k + 1] for k in range(top)]),
    ]
    for n, out in enumerate(outs):
        out[0:rows, :] = normed[:, n * chunk : (n + 1) * chunk]
    block = jnp.concatenate(lines + [jnp.zeros((META - len(lines), chunk), f32)], axis=0)
    outs[0][rows : rows + META, :] = block.astype(bf16)


def pick_kernel(sources, peers, cap, place, *refs):
    blocks, out, meta = refs[: CHUNKS * sources], refs[-2], refs[-1]
    rows = blocks[0].shape[0] - META
    chunk = blocks[0].shape[1]
    top = chunk // rows
    plane = peers * cap
    row_ids = iota((plane, rows), 0)
    picked = []
    for idx in range(sources):
        mine = blocks[CHUNKS * idx : CHUNKS * (idx + 1)]
        ma = mine[0][rows : rows + META, :].astype(f32)
        sel = jnp.zeros((plane, rows), jnp.bool_)
        lines = []
        for k in range(top):
            expert = ma[0:1, k * rows : (k + 1) * rows].astype(jnp.int32)
            rank = ma[1:2, k * rows : (k + 1) * rows].astype(jnp.int32)
            local = expert - place[2] * peers
            inside = (local >= 0) & (local < peers)
            slot = jnp.where(inside, local * cap + rank, -1)
            sel = sel | (row_ids == slot)
            lines.append(slot.astype(f32))
        for k in range(top):
            lines.append(ma[2:3, k * rows : (k + 1) * rows] + ma[3:4, k * rows : (k + 1) * rows])
        meta[idx * 2 * top : (idx + 1) * 2 * top, :] = jnp.concatenate(lines, axis=0)
        onehot = sel.astype(f32).astype(bf16)
        picked.append([jnp.dot(onehot, m[0:rows, :], preferred_element_type=f32) for m in mine])
    for p in range(peers):
        for n in range(CHUNKS):
            column = [picked[i][n][p * cap : (p + 1) * cap, :] for i in range(sources)]
            out[p, :, n * chunk : (n + 1) * chunk] = jnp.concatenate(column, axis=0).astype(bf16)


def expert_kernel(place, arrived, *refs):
    weights, out, slots, sems = refs[:6], refs[6], refs[7:13], refs[13]
    core = place[0]
    copies = []
    for n in range(6):
        copies.append(pltpu.make_async_copy(weights[n].at[core], slots[n], sems.at[n]))
        copies[-1].start()
    peers, rows, _ = arrived.shape
    x = jnp.concatenate([arrived[p] for p in range(peers)], axis=0)
    hidden = []
    for h in range(2):
        copies[3 * h].wait()
        gate = jnp.dot(x, slots[3 * h][...], preferred_element_type=f32)
        copies[3 * h + 1].wait()
        up = jnp.dot(x, slots[3 * h + 1][...], preferred_element_type=f32)
        hidden.append((gate / (1.0 + jnp.exp(-gate)) * up).astype(bf16))
    copies[2].wait()
    copies[5].wait()
    y = jnp.dot(hidden[0], slots[2][...], preferred_element_type=f32)
    y = y + jnp.dot(hidden[1], slots[5][...], preferred_element_type=f32)
    y = y.astype(bf16)
    for p in range(peers):
        out[p] = y[p * rows : (p + 1) * rows, :]


def mix_kernel(sources, cap, returned, meta, *outs):
    rows = meta.shape[1]
    lines = meta.shape[0] // sources
    top = lines // 2
    chunk = outs[0].shape[1]
    peers = returned.shape[0]
    row_ids = iota((peers * cap, rows), 0)
    for idx in range(sources):
        m = meta[idx * lines : (idx + 1) * lines, :]
        w = jnp.zeros((peers * cap, rows), f32)
        for k in range(top):
            w = w + jnp.where(
                row_ids == m[k : k + 1, :].astype(jnp.int32), m[top + k : top + k + 1, :], 0.0
            )
        high = w.astype(bf16)
        low = (w - high.astype(f32)).astype(bf16)
        wt = jnp.concatenate([high, low], axis=0)
        y = jnp.concatenate(
            [returned[p, idx * cap : (idx + 1) * cap, :].astype(f32) for p in range(peers)], axis=0
        ).astype(bf16)
        y = jnp.concatenate([y, y], axis=0)
        part = lax.dot_general(wt, y, (((0,), (0,)), ((), ())), preferred_element_type=f32)
        for n in range(CHUNKS):
            out = outs[CHUNKS * idx + n]
            out[...] = part[:, n * chunk : (n + 1) * chunk].astype(out.dtype)


def shifted(value, axis, by):
    count = lax.axis_size(axis)
    return lax.ppermute(value, axis, [(i, (i + by) % count) for i in range(count)])


def moved(value, to):
    planes, cores = lax.axis_size("z"), lax.axis_size("tp")
    pairs = []
    for z in range(planes):
        for t in range(cores):
            there, core = to(z, t)
            pairs.append((z * cores + t, there % planes * cores + core))
    return lax.ppermute(value, ("z", "tp"), pairs)


def exchanged(value):
    return lax.all_to_all(value, ("x", "tp"), split_axis=0, concat_axis=0, tiled=True)


def body(tokens, in_gain, routing, gate_prob, w_gate, w_up, w_down, out_gain):
    planes = lax.axis_size("z")
    xs = lax.axis_size("x")
    cores = lax.axis_size("tp")
    peers = xs * cores
    local_experts = w_gate.shape[0]
    expert_count = local_experts * planes * xs
    rows, top = routing.shape
    width = tokens.shape[1]
    chunk = width // CHUNKS
    cap = max(2, rows * top // (2 * (expert_count // GROUPS)))
    core = lax.axis_index("tp")
    place = jnp.stack([core, lax.axis_index("x"), lax.axis_index("z")]).astype(jnp.int32)

    weights = (w_gate, w_up, w_down)
    theirs = tuple(shifted(w, "tp", 1) for w in weights)

    blank = [jax.ShapeDtypeStruct((rows + (0 if n else META), chunk), bf16) for n in range(CHUNKS)]
    held = pl.pallas_call(
        functools.partial(prep_kernel, expert_count),
        out_shape=tuple(blank),
        in_specs=[VM, VM, VM, VM],
        out_specs=(VM,) * CHUNKS,
        name="prep",
        compiler_params=pltpu.CompilerParams(vmem_limit_bytes=LIMITS["prep"]),
    )(tokens, in_gain.reshape(1, width), routing.T, gate_prob.T)

    share = planes // cores
    blocks = []
    for step in range(share):
        if step == 0:
            held = [moved(v, lambda z, t: (z + t, t)) for v in held]
        else:
            held = [moved(v, lambda z, t: (z + 2 * t - 1, t)) for v in held]
        blocks.append(held)
    near = list(range(NEAR))
    far = list(range(NEAR, share))

    def pick(offsets):
        count = len(offsets)
        return pl.pallas_call(
            functools.partial(pick_kernel, count, peers, cap),
            out_shape=(
                jax.ShapeDtypeStruct((peers, count * cap, width), bf16),
                jax.ShapeDtypeStruct((count * 2 * top, rows), f32),
            ),
            in_specs=[SM] + [VM] * (CHUNKS * count),
            out_specs=(VM, VM),
            name="pick",
            compiler_params=pltpu.CompilerParams(vmem_limit_bytes=LIMITS["pick"]),
        )(place, *[b for o in offsets for b in blocks[o]])

    def expert(arrived):
        shapes = [w.shape[1:] for w in weights] * 2
        return pl.pallas_call(
            expert_kernel,
            out_shape=jax.ShapeDtypeStruct(arrived.shape, bf16),
            in_specs=[SM, VM] + [HB] * 6,
            out_specs=VM,
            scratch_shapes=[pltpu.VMEM(s, bf16) for s in shapes] + [pltpu.SemaphoreType.DMA((6,))],
            name="expert",
            compiler_params=pltpu.CompilerParams(vmem_limit_bytes=LIMITS["expert"]),
        )(place, arrived, *weights, *theirs)

    parts = {}

    def mix(offsets, returned, meta):
        count = len(offsets)
        keys = [(o, n) for o in offsets for n in range(CHUNKS)]
        made = pl.pallas_call(
            functools.partial(mix_kernel, count, cap),
            out_shape=tuple(
                jax.ShapeDtypeStruct((rows, chunk), bf16 if k[0] == share - 1 else f32) for k in keys
            ),
            in_specs=[VM, VM],
            out_specs=(VM,) * (CHUNKS * count),
            name="mix",
            compiler_params=pltpu.CompilerParams(vmem_limit_bytes=LIMITS["mix" if 0 in offsets else "far_mix"]),
        )(returned, meta)
        parts.update(zip(keys, made))

    near_rows, near_meta = pick(near)
    near_rows = exchanged(near_rows)
    far_rows, far_meta = pick(far)
    far_rows = exchanged(far_rows)
    near_out = expert(near_rows)
    far_out = expert(far_rows)
    far_back = exchanged(far_out)
    near_back = exchanged(near_out)
    mix(far, far_back, far_meta)
    mix(near, near_back, near_meta)

    flows = [parts[share - 1, n] for n in range(CHUNKS)]
    for step in range(1, share):
        for n in range(CHUNKS):
            value = moved(flows[n], lambda z, t: (z + 1 - 2 * t, t))
            flows[n] = (value.astype(f32) + parts[share - 1 - step, n]).astype(bf16)
    sums = []
    for n in range(CHUNKS // 2):
        low, high = flows[n], flows[n + CHUNKS // 2]
        keep = moved(jnp.where(core == 0, low, high), lambda z, t: (z - t, t))
        give = moved(jnp.where(core == 0, high, low), lambda z, t: (z - t, 1 - t))
        sums.append(keep.astype(f32) + give.astype(f32))

    squares = sum(jnp.sum(s * s, axis=1) for s in sums)
    total = lax.all_gather(squares, "tp").sum(axis=0)
    scale = lax.rsqrt(total / width + EPS)[:, None]
    mixed = jnp.concatenate(sums, axis=1)
    return (mixed * scale * out_gain).astype(bf16)


def solution(mesh):
    grp, _, tp = mesh.axis_names
    groups, columns, cores = mesh.devices.shape
    split = Mesh(
        mesh.devices.reshape(groups, columns // X_CHIPS, X_CHIPS, cores), (grp, "z", "x", tp)
    )
    lines = (grp, "z", "x")
    spread = ("z", "x")
    placed = (
        P(lines, None),
        P(),
        P(lines, None),
        P(lines, None),
        P(spread, None, tp),
        P(spread, None, tp),
        P(spread, tp, None),
        P(tp),
    )


    return jax.shard_map(body, mesh=split, in_specs=placed, out_specs=P(lines, tp), check_vma=False)
```
